32 devices in a mesh: fs: 8 (over z, y), tp: 4 (over x, core).
Axes of the slice: x: 2, y: 2, z: 4, core: 2. Of those that a mesh axis runs over, the one named last changes fastest.
Arguments:
- hidden_states: bfloat16 [2048, 2048], P('tp', 'fs'), may hold values from -6 to 6
- norm_gain: float32 [2048], P('fs'), may hold values from 0.1 to 1.9
- gate_master: float32 [8, 2048, 7168], P(None, 'fs', 'tp'), may hold values from -0.125 to 0.125
- up_master: float32 [8, 2048, 7168], P(None, 'fs', 'tp'), may hold values from -0.125 to 0.125
- down_master: float32 [8, 2048, 7168], P(None, 'fs', 'tp'), may hold values from -0.0625 to 0.0625
- expert_ids: int32 [2048, 2], P('tp'), may hold values from 0 to 7, all different within a row; in each aligned block of 512 rows (0 to 511, 512 to 1023, ...) at most 256 rows name the same one
- route_logits: float32 [2048, 2], P('tp'), may hold values from -6 to 6
Outputs:
- gate_serve: bfloat16 [8, 2048, 7168], P('tp', None, 'fs')
- up_serve: bfloat16 [8, 2048, 7168], P('tp', None, 'fs')
- down_serve: bfloat16 [8, 2048, 7168], P('tp', None, 'fs')
- combined: bfloat16 [2048, 2048], P('tp', 'fs')
The draws below stay inside these ranges and needn't reach their ends.
Inputs may be any that keep to these rules, and one draw needn't show every extreme that they name: `expert_ids`: the 2 entries of a row differ. Among the rows of one index of tp (aligned blocks of 512 rows) no expert is named more than 256 times, and in some blocks one expert is named exactly 256 times.
All inputs are finite; a program needn't handle non-finite values.
Results may differ from the reference program's by a relative error of at most 0.018.
Values may be sent and summed in bfloat16 or wider, within the bound.
A program may use at most 192 MiB of HBM per device.

```python
import math
import jax
import jax.numpy as jnp
import numpy as np
from jax import lax

D = 2048
FF = 7168
EXPERTS = 8
TOP = 2
TOK_DEV = 512
CAP = 256
TOKENS = 2048


def levels(key, dims, shards, smallest, largest):
    def one(axis_at, blocks):
        steps = jax.random.uniform(jax.random.fold_in(jax.random.fold_in(key, 6), axis_at), (blocks,), jnp.float32, smallest / len(shards), largest / len(shards))
        return jnp.repeat(jnp.exp(steps), dims[axis_at] // blocks).reshape((-1,) + (1,) * (len(dims) - axis_at - 1))

    loudness = one(*shards[0])
    for cut in shards[1:]:
        loudness = loudness * one(*cut)
    return loudness


def shared_out(key, own, number, rows, amount, top, bound, slope):
    sequence = jax.random.permutation(key, amount)
    heavy_load, ordinary = load_shares(amount, rows * top, bound, slope, True), load_shares(amount, rows * top, bound, slope, False)
    places = jnp.arange(amount)

    def named(lengths, offset_by):
        used = int((lengths > 0).sum())
        fixed = max(1, used // 4)
        passed = fixed + (places - fixed + offset_by * (used - fixed)) % max(1, amount - fixed)
        return jnp.zeros((amount,), jnp.int32).at[sequence[jnp.where(places < fixed, places, passed)]].set(jnp.asarray(lengths, jnp.int32))

    lengths = jnp.where(number % 4 == 0, named(heavy_load, number // 4), named(ordinary, number - number // 4 - 1))
    mixed = jax.random.permutation(jax.random.fold_in(own, 3), amount)
    donor, taker = mixed[0:amount // 2 * 2:2], mixed[1:amount // 2 * 2:2]
    room = jnp.minimum(lengths[donor] - 1, bound - lengths[taker]) // 2
    room = jnp.where((donor == sequence[0]) | (taker == sequence[0]) | (lengths[taker] == 0), 0, jnp.maximum(room, 0))
    passed = jax.random.randint(jax.random.fold_in(own, 4), (amount // 2,), 0, 1 << 20) % (room + 1)
    lengths = lengths.at[donor].add(-passed).at[taker].add(passed)
    labels = jnp.searchsorted(jnp.cumsum(lengths), jnp.arange(rows * top), side="right").astype(jnp.int32)
    listing = labels.reshape(top, rows).T
    listing = listing[jax.random.permutation(jax.random.fold_in(own, 1), rows)]
    offset_by = jax.random.randint(jax.random.fold_in(own, 2), (rows, 1), 0, top)
    return jnp.take_along_axis(listing, (jnp.arange(top)[None, :] + offset_by) % top, axis=1)


def load_shares(amount, total, limit, lean, full):
    loads = [(1 << 20) // math.isqrt(rank ** lean) + 1 for rank in range(1, amount + 1)]
    largest = limit if full else min(limit, max(-(-total // amount), total * loads[0] // sum(loads)))
    least = 1 if total - largest >= amount - 1 else 0
    counts, spare = [largest] + [least] * (amount - 1), total - largest - least * (amount - 1)
    while spare > 0:
        candidates = [i for i in range(1, amount) if counts[i] < largest] or [i for i in range(1, amount) if counts[i] < limit]
        whole, left = sum([loads[i] for i in candidates]), spare
        for i in candidates:
            extra = min(limit - counts[i], max(1, left * loads[i] // whole), spare)
            counts[i] = counts[i] + extra
            spare = spare - extra
    return np.array(counts)


def scatter_about(key, extent, deviation, limit, shards=(), kind=jnp.bfloat16):
    array = deviation * jax.random.normal(key, extent, jnp.float32)
    if shards:
        array = array * levels(key, extent, shards, -0.22, 0.18)
    return jnp.clip(array, -limit, limit).astype(kind)


def setup_inputs(seed: int = 0) -> dict:
    keys = jax.random.split(jax.random.key(seed), 8)
    hidden_states = scatter_about(keys[0], (TOKENS, D), 1.0, 6.0, ((0, 4), (1, 8)))
    norm_gain = jnp.clip(1.0 + 0.18 * jax.random.normal(keys[1], (D,), jnp.float32), 0.1, 1.9)
    gate_master = scatter_about(keys[2], (EXPERTS, D, FF), D ** -0.5, 0.125, ((1, 8), (2, 4)), jnp.float32)
    up_master = scatter_about(keys[3], (EXPERTS, D, FF), D ** -0.5, 0.125, ((1, 8), (2, 4)), jnp.float32)
    down_master = scatter_about(keys[4], (EXPERTS, D, FF), FF ** -0.5, 0.0625, ((1, 8), (2, 4)), jnp.float32)
    expert_ids_keys = jax.random.split(jax.random.fold_in(keys[5], 1), TOKENS // TOK_DEV)
    expert_ids_turns = jax.random.permutation(jax.random.fold_in(keys[5], 3), TOKENS // TOK_DEV)
    expert_ids = jax.vmap(lambda own, number: shared_out(jax.random.fold_in(keys[5], 2), own, number, TOK_DEV, EXPERTS, TOP, CAP, 2))(expert_ids_keys, expert_ids_turns).reshape((TOKENS, TOP))
    route_logits = scatter_about(keys[6], (TOKENS, TOP), 1.0, 6.0, ((0, 4),), jnp.float32)
    return {"hidden_states": hidden_states, "norm_gain": norm_gain, "gate_master": gate_master, "up_master": up_master, "down_master": down_master, "expert_ids": expert_ids, "route_logits": route_logits}


EPSILON = 1e-06

def reference(hidden_states, norm_gain, gate_master, up_master, down_master, expert_ids, route_logits):
    scaled = norm_gain[None, :, None]
    gate_serve = (scaled * gate_master).astype(jnp.bfloat16)
    up_serve = (scaled * up_master).astype(jnp.bfloat16)
    down_serve = down_master.astype(jnp.bfloat16)
    values = hidden_states.astype(jnp.float32)
    inv_rms = lax.rsqrt(lax.optimization_barrier(jnp.mean(values * values, axis=1, keepdims=True)) + EPSILON)
    normed = (values * inv_rms).astype(jnp.bfloat16)
    route_weight = jax.nn.softmax(route_logits, axis=1)

    def expert_output(expert):
        gate_pre = jnp.dot(normed, gate_serve[expert], preferred_element_type=jnp.float32)
        up_pre = jnp.dot(normed, up_serve[expert], preferred_element_type=jnp.float32)
        act = (jax.nn.silu(gate_pre) * up_pre).astype(jnp.bfloat16)
        return jnp.dot(act, down_serve[expert].T, preferred_element_type=jnp.float32).astype(jnp.bfloat16)
    outputs = lax.map(expert_output, jnp.arange(EXPERTS, dtype=jnp.int32))
    by_token = jnp.transpose(outputs, (1, 0, 2))
    picked = jnp.take_along_axis(by_token, expert_ids[:, :, None].astype(jnp.int32), axis=1)
    combined = lax.optimization_barrier(jnp.sum(route_weight[:, :, None] * picked.astype(jnp.float32), axis=1)).astype(jnp.bfloat16)
    return (gate_serve, up_serve, down_serve, combined)
```

```python
import functools

import jax
import jax.numpy as jnp
from jax import lax
from jax.experimental import pallas as pl
from jax.experimental.pallas import tpu as pltpu
from jax.sharding import PartitionSpec as P

EPSILON = 1e-06
SLOTS = 4
MESH = pl.DeviceIdType.MESH


def exchange_kernel(
    groups, row_groups, expert, chunks, gain_ref, gate_ref, up_ref, down_ref, dep_ref,
    gate_out, up_out, down_out, stage, cast, landed, load_sem,
    send_a, recv_a, send_b, recv_b,
):
    me = lax.axis_index("tp")
    row = lax.axis_index("fs")
    blocks = row_groups // groups
    masters = (gate_ref, up_ref, down_ref)
    outs = (gate_out, up_out, down_out)
    local_count = gate_ref.shape[0] // groups
    rows, columns = gate_ref.shape[1:]
    height = rows // chunks
    width = columns // blocks

    barrier = pltpu.get_barrier_semaphore()
    for step in range(1, groups):
        pl.semaphore_signal(
            barrier, inc=1, device_id={"tp": lax.rem(me + step, groups)}, device_id_type=MESH
        )
    for step in range(1, row_groups):
        pl.semaphore_signal(
            barrier, inc=1, device_id={"fs": lax.rem(row + step, row_groups)}, device_id_type=MESH
        )
    order = [groups // 2] + [s for s in range(1, groups) if s != groups // 2] + [0]
    units = [(w, c) for w in range(len(masters)) for c in range(chunks)]
    jobs = [(u, s) for u in range(len(units)) for s in order]

    def load(n):
        u, s = jobs[n]
        w, c = units[u]
        number = lax.rem(me + s, groups) * local_count + expert
        return pltpu.make_async_copy(
            masters[w].at[number, pl.ds(c * height, height)],
            stage.at[n % SLOTS],
            load_sem.at[n % SLOTS],
        )

    for n in range(SLOTS):
        load(n).start()
    pl.semaphore_wait(barrier, groups - 1 + row_groups - 1)

    def first(u, s):
        return pltpu.make_async_remote_copy(
            src_ref=cast.at[u, s],
            dst_ref=landed.at[u, s - 1],
            send_sem=send_a.at[u, s - 1],
            recv_sem=recv_a.at[u, s - 1],
            device_id={"tp": lax.rem(me + s, groups)},
            device_id_type=MESH,
        )

    def place(u, source):
        w, c = units[u]
        start = pl.multiple_of(source * rows + c * height, height)
        return outs[w].at[pl.ds(start, height)]

    def second(u, s, b):
        held = cast.at[u, 0] if s == 0 else landed.at[u, s - 1]
        goal = lax.rem(me + groups - s, groups) * blocks + b
        piece = held.at[:, pl.ds(b * width, width)]
        remote = lambda: pltpu.make_async_remote_copy(
            src_ref=piece,
            dst_ref=place(u, row),
            send_sem=send_b.at[u, s * blocks + b],
            recv_sem=recv_b.at[u, row],
            device_id={"fs": goal},
            device_id_type=MESH,
        )
        local = lambda: pltpu.make_async_copy(piece, place(u, row), recv_b.at[u, row])
        return goal, remote, local

    def pass_on(u, s):
        for b in range(blocks):
            goal, remote, local = second(u, s, b)

            @pl.when(goal != row)
            def _():
                remote().start()

            @pl.when(goal == row)
            def _():
                local().start()

    def forward(u):
        for s in sorted(range(1, groups), key=lambda s: s == groups // 2):
            first(u, s).wait_recv()
            pass_on(u, s)

    strip = 16
    for n, (u, s) in enumerate(jobs):
        w, c = units[u]
        load(n).wait()
        slot = n % SLOTS

        def convert(i, carry):
            at = pl.ds(pl.multiple_of(i * strip, strip), strip)
            value = stage[slot, at, :]
            if w < 2:
                gain = gain_ref[pl.ds(pl.multiple_of(c * height + i * strip, strip), strip), :]
                value = value * gain
            cast[u, s, at, :] = value.astype(jnp.bfloat16)
            return carry

        lax.fori_loop(0, height // strip, convert, 0)
        if n + SLOTS < len(jobs):
            load(n + SLOTS).start()
        if s == 0:
            pass_on(u, 0)
            if u >= 1:
                forward(u - 1)
        else:
            first(u, s).start()
    forward(len(units) - 1)
    for u in range(len(units)):
        for s in range(groups):
            if s:
                first(u, s).wait_send()
            for b in range(blocks):
                goal, remote, local = second(u, s, b)

                @pl.when(goal != row)
                def _():
                    remote().wait_send()
        for source in range(row_groups):
            pltpu.make_async_copy(
                cast.at[u, 0, :, pl.ds(0, width)], place(u, source), recv_b.at[u, source]
            ).wait()


def exchange(gain, gate, up, down, dep, expert, collective):
    groups = lax.axis_size("tp")
    row_groups = lax.axis_size("fs")
    experts, rows, columns = gate.shape
    blocks = row_groups // groups
    width = columns // blocks
    chunks = 2
    units = 3 * chunks
    height = rows // chunks
    out = jax.ShapeDtypeStruct((rows * row_groups, width), jnp.bfloat16)
    hbm = pl.BlockSpec(memory_space=pl.ANY)
    sent = 3 * rows * columns * 2 * groups
    return pl.pallas_call(
        functools.partial(exchange_kernel, groups, row_groups, expert, chunks),
        out_shape=(out, out, out),
        in_specs=[pl.BlockSpec(memory_space=pltpu.VMEM), hbm, hbm, hbm, hbm],
        out_specs=(hbm, hbm, hbm),
        scratch_shapes=[
            pltpu.VMEM((SLOTS, height, columns), jnp.float32),
            pltpu.VMEM((units, groups, height, columns), jnp.bfloat16),
            pltpu.VMEM((units, groups - 1, height, columns), jnp.bfloat16),
            pltpu.SemaphoreType.DMA((SLOTS,)),
            pltpu.SemaphoreType.DMA((units, groups - 1)),
            pltpu.SemaphoreType.DMA((units, groups - 1)),
            pltpu.SemaphoreType.DMA((units, row_groups)),
            pltpu.SemaphoreType.DMA((units, row_groups)),
        ],
        compiler_params=pltpu.CompilerParams(
            collective_id=collective, has_side_effects=True, vmem_limit_bytes=44 * 1024 * 1024
        ),
        cost_estimate=pl.CostEstimate(
            flops=rows * columns, bytes_accessed=32 * sent, transcendentals=0
        ),
    )(gain, gate, up, down, dep)


def fused_device(
    hidden_states, norm_gain, gate_master, up_master, down_master, expert_ids, route_logits
):
    groups = lax.axis_size("tp")
    row_groups = lax.axis_size("fs")
    experts = gate_master.shape[0]
    local_count = experts // groups
    tokens, pieces = hidden_states.shape
    model_width = pieces * row_groups
    capacity = tokens // 2
    me = lax.axis_index("tp")
    gain = norm_gain[:, None]
    raw = lax.all_gather(hidden_states, "fs", axis=1, tiled=True)
    raw = lax.all_gather(raw, "tp", axis=0)
    all_ids = lax.all_gather(expert_ids, "tp", axis=0)
    earlier = (jnp.arange(tokens)[:, None] > jnp.arange(tokens)[None, :]).astype(jnp.bfloat16)
    weights = jax.nn.softmax(route_logits, axis=1)
    named = expert_ids[:, :, None] == jnp.arange(experts, dtype=jnp.int32)[None, None, :]
    chosen = jnp.any(named, axis=1).astype(jnp.bfloat16)
    before = jnp.dot(earlier, chosen, preferred_element_type=jnp.float32)
    position = jnp.sum(jnp.where(named, before[:, None, :], 0.0), axis=2).astype(jnp.int32)
    slot_ids = (expert_ids * capacity + position).reshape(-1)

    dep = hidden_states
    served = []
    partials = []
    for j in range(local_count):
        gate, up, down = exchange(gain, gate_master, up_master, down_master, dep, j, 1 + j)
        served.append((gate, up, down))
        mine = jnp.any(all_ids == me * local_count + j, axis=2)
        spot = jnp.einsum(
            "ts,gs->gt", earlier, mine.astype(jnp.bfloat16), preferred_element_type=jnp.float32
        ).astype(jnp.int32)
        table = (
            mine[:, None, :]
            & (spot[:, None, :] == jnp.arange(capacity, dtype=jnp.int32)[None, :, None])
        ).astype(jnp.bfloat16)
        packed = jnp.einsum("gct,gtd->gcd", table, raw, preferred_element_type=jnp.float32)
        packed = packed.reshape(groups * capacity, model_width)
        mean = jnp.mean(packed * packed, axis=1, keepdims=True)
        normed = (packed * lax.rsqrt(mean + EPSILON)).astype(jnp.bfloat16)
        gate_pre = jnp.dot(normed, gate, preferred_element_type=jnp.float32)
        up_pre = jnp.dot(normed, up, preferred_element_type=jnp.float32)
        act = (jax.nn.silu(gate_pre) * up_pre).astype(jnp.bfloat16)
        partial = jnp.einsum(
            "dh,sh->ds", down, act, preferred_element_type=jnp.float32
        ).astype(jnp.bfloat16)
        partials.append(partial)
        dep = partial
    returned = []
    for partial in partials:
        summed = lax.psum_scatter(partial, "fs", scatter_dimension=0, tiled=True)
        returned.append(
            lax.all_to_all(
                summed.reshape(pieces, groups, capacity), "tp", split_axis=1, concat_axis=1, tiled=True
            )
        )
    flat_out = jnp.stack(returned, axis=2).reshape(pieces, experts * capacity)
    picked = flat_out.at[:, slot_ids].get(mode="promise_in_bounds")
    picked = picked.reshape(pieces, tokens, 2).astype(jnp.float32)
    combined = jnp.sum(picked * weights[None, :, :], axis=2)
    return tuple(jnp.stack([one[w] for one in served]) for w in range(3)) + (
        jnp.transpose(combined).astype(jnp.bfloat16),
    )


def arrange(weights, groups, row_groups):
    experts, rows, columns = weights.shape
    blocks = row_groups // groups
    split = weights.reshape(experts // groups, groups, rows, blocks, columns // blocks)
    split = split.reshape(groups, experts // groups, rows, blocks, columns // blocks)
    return jnp.transpose(split, (0, 3, 1, 2, 4))


def regroup(moved, row_groups):
    return moved.reshape((row_groups,) + moved.shape[2:])


def settle(arrived):
    return arrived.reshape(arrived.shape[1], arrived.shape[2], arrived.shape[3])


def per_device(
    hidden_states, norm_gain, gate_master, up_master, down_master, expert_ids, route_logits
):
    groups = lax.axis_size("tp")
    row_groups = lax.axis_size("fs")
    whole_tiles = gate_master.shape[2] // (row_groups // groups) % 128 == 0
    if whole_tiles and gate_master.shape[1] % 256 == 0:
        return fused_device(
            hidden_states, norm_gain, gate_master, up_master, down_master, expert_ids, route_logits
        )
    experts = gate_master.shape[0]
    local_count = experts // groups
    tokens = hidden_states.shape[0]
    pieces = hidden_states.shape[1]
    model_width = pieces * row_groups
    capacity = tokens // 2
    scaled = norm_gain[None, :, None]
    gate_cast = arrange((scaled * gate_master).astype(jnp.bfloat16), groups, row_groups)
    up_cast = arrange((scaled * up_master).astype(jnp.bfloat16), groups, row_groups)
    down_cast = arrange(down_master.astype(jnp.bfloat16), groups, row_groups)
    sectioned = (
        lax.all_to_all(gate_cast, "tp", split_axis=0, concat_axis=0, tiled=True),
        lax.all_to_all(up_cast, "tp", split_axis=0, concat_axis=0, tiled=True),
        lax.all_to_all(down_cast, "tp", split_axis=0, concat_axis=0, tiled=True),
    )
    landed = (
        lax.all_to_all(
            regroup(sectioned[0], row_groups), "fs", split_axis=0, concat_axis=2, tiled=True
        ),
        lax.all_to_all(
            regroup(sectioned[1], row_groups), "fs", split_axis=0, concat_axis=2, tiled=True
        ),
        lax.all_to_all(
            regroup(sectioned[2], row_groups), "fs", split_axis=0, concat_axis=2, tiled=True
        ),
    )
    gate_serve, up_serve, down_serve = (settle(landed[0]), settle(landed[1]), settle(landed[2]))
    values = hidden_states.astype(jnp.float32)
    squares = lax.psum(jnp.sum(values * values, axis=1), "fs")
    normed = (values * lax.rsqrt(squares / model_width + EPSILON)[:, None]).astype(jnp.bfloat16)
    weights = jax.nn.softmax(route_logits, axis=1)
    chosen = (expert_ids[:, :, None] == jnp.arange(experts, dtype=jnp.int32)[None, None, :]).astype(
        jnp.int32
    )
    chosen = chosen.reshape(tokens * 2, experts)
    before = jnp.cumsum(chosen, axis=0) - chosen
    position = jnp.sum(before * chosen, axis=1)
    slot_ids = expert_ids.reshape(-1) * capacity + position
    slot_table = (
        slot_ids[None, :] == jnp.arange(experts * capacity, dtype=jnp.int32)[:, None]
    ).astype(jnp.bfloat16)
    dispatch = jnp.sum(slot_table.reshape(experts * capacity, tokens, 2), axis=2)
    whole_rows = lax.all_gather(normed, "fs", axis=1, tiled=True)
    packed = jnp.dot(dispatch, whole_rows, preferred_element_type=jnp.float32).astype(jnp.bfloat16)
    arrived = lax.all_to_all(
        packed.reshape(groups, local_count * capacity, model_width),
        "tp",
        split_axis=0,
        concat_axis=0,
        tiled=True,
    )
    arranged = arrived.reshape(groups, local_count, capacity, model_width)
    activations = []
    for expert_index in range(local_count):
        expert_rows = arranged[:, expert_index].reshape(groups * capacity, model_width)
        gate_pre = jnp.dot(
            expert_rows, gate_serve[expert_index], preferred_element_type=jnp.float32
        )
        up_pre = jnp.dot(expert_rows, up_serve[expert_index], preferred_element_type=jnp.float32)
        activations.append((jax.nn.silu(gate_pre) * up_pre).astype(jnp.bfloat16))
    stacked = jnp.stack(activations)
    summed = lax.psum_scatter(
        jnp.einsum("jdh,jsh->djs", down_serve, stacked, preferred_element_type=jnp.float32).astype(
            jnp.bfloat16
        ),
        "fs",
        scatter_dimension=0,
        tiled=True,
    )
    results = summed.reshape(pieces, local_count, groups, capacity)
    returned = lax.all_to_all(results, "tp", split_axis=2, concat_axis=1, tiled=True)
    flat_out = returned.reshape(pieces, experts * capacity)
    picked = jnp.take(flat_out, slot_ids, axis=1).reshape(pieces, tokens, 2).astype(jnp.float32)
    combined = jnp.sum(picked * weights[None, :, :], axis=2)
    return (gate_serve, up_serve, down_serve, jnp.transpose(combined).astype(jnp.bfloat16))


def solution(mesh):
    in_specs = (
        P("tp", "fs"),
        P("fs"),
        P(None, "fs", "tp"),
        P(None, "fs", "tp"),
        P(None, "fs", "tp"),
        P("tp", None),
        P("tp", None),
    )
    out_specs = (P("tp", None, "fs"), P("tp", None, "fs"), P("tp", None, "fs"), P("tp", "fs"))
    return jax.shard_map(
        per_device, mesh=mesh, in_specs=in_specs, out_specs=out_specs, check_vma=False
    )
```

```python
import functools

import jax
import jax.numpy as jnp
from jax import lax
from jax.experimental import pallas as pl
from jax.experimental.pallas import tpu as pltpu
from jax.sharding import PartitionSpec as P

EPSILON = 1e-06
SLOTS = 4
MESH = pl.DeviceIdType.MESH


def exchange_kernel(
    groups, row_groups, expert, chunks, gain_ref, gate_ref, up_ref, down_ref, dep_ref,
    gate_out, up_out, down_out, stage, cast, landed, load_sem,
    send_a, recv_a, send_b, recv_b,
):
    me = lax.axis_index("tp")
    row = lax.axis_index("fs")
    blocks = row_groups // groups
    masters = (gate_ref, up_ref, down_ref)
    outs = (gate_out, up_out, down_out)
    local_count = gate_ref.shape[0] // groups
    rows, columns = gate_ref.shape[1:]
    height = rows // chunks
    width = columns // blocks

    barrier = pltpu.get_barrier_semaphore()
    for step in range(1, groups):
        pl.semaphore_signal(
            barrier, inc=1, device_id={"tp": lax.rem(me + step, groups)}, device_id_type=MESH
        )
    for step in range(1, row_groups):
        pl.semaphore_signal(
            barrier, inc=1, device_id={"fs": lax.rem(row + step, row_groups)}, device_id_type=MESH
        )
    order = [groups // 2] + [s for s in range(1, groups) if s != groups // 2] + [0]
    units = [(w, c) for w in range(len(masters)) for c in range(chunks)]
    jobs = [(u, s) for u in range(len(units)) for s in order]

    def load(n):
        u, s = jobs[n]
        w, c = units[u]
        number = lax.rem(me + s, groups) * local_count + expert
        return pltpu.make_async_copy(
            masters[w].at[number, pl.ds(c * height, height)],
            stage.at[n % SLOTS],
            load_sem.at[n % SLOTS],
        )

    for n in range(SLOTS):
        load(n).start()
    pl.semaphore_wait(barrier, groups - 1 + row_groups - 1)

    def first(u, s):
        return pltpu.make_async_remote_copy(
            src_ref=cast.at[u, s],
            dst_ref=landed.at[u, s - 1],
            send_sem=send_a.at[u, s - 1],
            recv_sem=recv_a.at[u, s - 1],
            device_id={"tp": lax.rem(me + s, groups)},
            device_id_type=MESH,
        )

    def place(u, source):
        w, c = units[u]
        start = pl.multiple_of(source * rows + c * height, height)
        return outs[w].at[pl.ds(start, height)]

    def second(u, s, b):
        held = cast.at[u, 0] if s == 0 else landed.at[u, s - 1]
        goal = lax.rem(me + groups - s, groups) * blocks + b
        piece = held.at[:, pl.ds(b * width, width)]
        remote = lambda: pltpu.make_async_remote_copy(
            src_ref=piece,
            dst_ref=place(u, row),
            send_sem=send_b.at[u, s * blocks + b],
            recv_sem=recv_b.at[u, row],
            device_id={"fs": goal},
            device_id_type=MESH,
        )
        local = lambda: pltpu.make_async_copy(piece, place(u, row), recv_b.at[u, row])
        return goal, remote, local

    def pass_on(u, s):
        for b in range(blocks):
            goal, remote, local = second(u, s, b)

            @pl.when(goal != row)
            def _():
                remote().start()

            @pl.when(goal == row)
            def _():
                local().start()

    def forward(u):
        for s in sorted(range(1, groups), key=lambda s: s == groups // 2):
            first(u, s).wait_recv()
            pass_on(u, s)

    strip = 16
    for n, (u, s) in enumerate(jobs):
        w, c = units[u]
        load(n).wait()
        slot = n % SLOTS

        def convert(i, carry):
            at = pl.ds(pl.multiple_of(i * strip, strip), strip)
            value = stage[slot, at, :]
            if w < 2:
                gain = gain_ref[pl.ds(pl.multiple_of(c * height + i * strip, strip), strip), :]
                value = value * gain
            cast[u, s, at, :] = value.astype(jnp.bfloat16)
            return carry

        lax.fori_loop(0, height // strip, convert, 0)
        if n + SLOTS < len(jobs):
            load(n + SLOTS).start()
        if s == 0:
            pass_on(u, 0)
            if u >= 1:
                forward(u - 1)
        else:
            first(u, s).start()
    forward(len(units) - 1)
    for u in range(len(units)):
        for s in range(groups):
            if s:
                first(u, s).wait_send()
            for b in range(blocks):
                goal, remote, local = second(u, s, b)

                @pl.when(goal != row)
                def _():
                    remote().wait_send()
        for source in range(row_groups):
            pltpu.make_async_copy(
                cast.at[u, 0, :, pl.ds(0, width)], place(u, source), recv_b.at[u, source]
            ).wait()


def exchange(gain, gate, up, down, dep, expert, collective):
    groups = lax.axis_size("tp")
    row_groups = lax.axis_size("fs")
    experts, rows, columns = gate.shape
    blocks = row_groups // groups
    width = columns // blocks
    chunks = 2
    units = 3 * chunks
    height = rows // chunks
    out = jax.ShapeDtypeStruct((rows * row_groups, width), jnp.bfloat16)
    hbm = pl.BlockSpec(memory_space=pl.ANY)
    sent = 3 * rows * columns * 2 * groups
    return pl.pallas_call(
        functools.partial(exchange_kernel, groups, row_groups, expert, chunks),
        out_shape=(out, out, out),
        in_specs=[pl.BlockSpec(memory_space=pltpu.VMEM), hbm, hbm, hbm, hbm],
        out_specs=(hbm, hbm, hbm),
        scratch_shapes=[
            pltpu.VMEM((SLOTS, height, columns), jnp.float32),
            pltpu.VMEM((units, groups, height, columns), jnp.bfloat16),
            pltpu.VMEM((units, groups - 1, height, columns), jnp.bfloat16),
            pltpu.SemaphoreType.DMA((SLOTS,)),
            pltpu.SemaphoreType.DMA((units, groups - 1)),
            pltpu.SemaphoreType.DMA((units, groups - 1)),
            pltpu.SemaphoreType.DMA((units, row_groups)),
            pltpu.SemaphoreType.DMA((units, row_groups)),
        ],
        compiler_params=pltpu.CompilerParams(
            collective_id=collective, has_side_effects=True, vmem_limit_bytes=44 * 1024 * 1024
        ),
        cost_estimate=pl.CostEstimate(
            flops=rows * columns, bytes_accessed=32 * sent, transcendentals=0
        ),
    )(gain, gate, up, down, dep)


def gather_sum_kernel(
    groups, row_groups, partial_ref, early_ref, out_ref, early_out, own, pair, summed, far, total,
    load_sem, send_a, recv_a, send_b, recv_b, send_c, recv_c, send_d, recv_d, early_sem,
):
    me = lax.axis_index("tp")
    row = lax.axis_index("fs")
    side = lax.rem(row, 2)
    mate = row + 1 - 2 * side
    stack = row_groups // 2
    level = row // 2
    pieces, slots = total.shape
    capacity = slots // groups

    barrier = pltpu.get_barrier_semaphore()
    for step in range(1, groups):
        pl.semaphore_signal(
            barrier, inc=1, device_id={"tp": lax.rem(me + step, groups)}, device_id_type=MESH
        )
    for step in range(1, row_groups):
        pl.semaphore_signal(
            barrier, inc=1, device_id={"fs": lax.rem(row + step, row_groups)}, device_id_type=MESH
        )
    order = [stack // 2] + [k for k in range(1, stack) if k != stack // 2] + [0]

    def rows_of(k, which):
        goal = lax.rem(level + k, stack) * 2 + which
        return partial_ref.at[pl.ds(pl.multiple_of(goal * pieces, pieces), pieces)]

    def load(k):
        return pltpu.make_async_copy(rows_of(k, side), own.at[k], load_sem.at[k])

    def across(k):
        return pltpu.make_async_remote_copy(
            src_ref=rows_of(k, 1 - side),
            dst_ref=pair.at[k],
            send_sem=send_a.at[k],
            recv_sem=recv_a.at[k],
            device_id={"fs": mate},
            device_id_type=MESH,
        )

    def along(k):
        return pltpu.make_async_remote_copy(
            src_ref=summed.at[k],
            dst_ref=far.at[k],
            send_sem=send_b.at[k],
            recv_sem=recv_b.at[k],
            device_id={"fs": lax.rem(level + k, stack) * 2 + side},
            device_id_type=MESH,
        )

    def back(s):
        goal = lax.rem(me + s, groups)
        columns = pl.ds(pl.multiple_of(goal * capacity, capacity), capacity)
        return pltpu.make_async_remote_copy(
            src_ref=total.at[:, columns],
            dst_ref=out_ref.at[me],
            send_sem=send_c.at[s - 1],
            recv_sem=recv_c.at[s - 1],
            device_id={"tp": goal},
            device_id_type=MESH,
        )

    def early_back(s):
        goal = lax.rem(me + s, groups)
        return pltpu.make_async_remote_copy(
            src_ref=early_ref.at[goal],
            dst_ref=early_out.at[me],
            send_sem=send_d.at[s - 1],
            recv_sem=recv_d.at[s - 1],
            device_id={"tp": goal},
            device_id_type=MESH,
        )

    for k in order:
        load(k).start()
    early_kept = pltpu.make_async_copy(early_ref.at[me], early_out.at[me], early_sem)
    pl.semaphore_wait(barrier, groups - 1 + row_groups - 1)
    for k in order:
        across(k).start()
    early_kept.start()
    for s in range(1, groups):
        early_back(s).start()
    strip = 16
    for k in order:
        load(k).wait()
        across(k).wait_recv()

        def add(i, carry):
            at = pl.ds(pl.multiple_of(i * strip, strip), strip)
            both = own[k, at, :].astype(jnp.float32) + pair[k, at, :].astype(jnp.float32)
            summed[k, at, :] = both.astype(jnp.bfloat16)
            return carry

        if k:
            lax.fori_loop(0, pieces // strip, add, 0)
            along(k).start()
    for k in range(1, stack):
        along(k).wait_recv()

    def finish(i, carry):
        at = pl.ds(pl.multiple_of(i * strip, strip), strip)
        value = own[0, at, :].astype(jnp.float32) + pair[0, at, :].astype(jnp.float32)
        for k in range(1, stack):
            value = value + far[k, at, :].astype(jnp.float32)
        total[at, :] = value.astype(jnp.bfloat16)
        return carry

    lax.fori_loop(0, pieces // strip, finish, 0)
    for s in range(1, groups):
        back(s).start()
    columns = pl.ds(pl.multiple_of(me * capacity, capacity), capacity)
    kept = pltpu.make_async_copy(total.at[:, columns], out_ref.at[me], load_sem.at[0])
    kept.start()
    kept.wait()
    early_kept.wait()
    for s in range(1, groups):
        early_back(s).wait()
        back(s).wait()
    for k in range(stack):
        across(k).wait_send()
        if k:
            along(k).wait_send()


def gather_sum(partial, early, collective):
    groups = lax.axis_size("tp")
    row_groups = lax.axis_size("fs")
    model_width, slots = partial.shape
    pieces = model_width // row_groups
    stack = row_groups // 2
    capacity = slots // groups
    block = pltpu.VMEM((stack, pieces, slots), jnp.bfloat16)
    sent = model_width * slots * 2
    return pl.pallas_call(
        functools.partial(gather_sum_kernel, groups, row_groups),
        out_shape=(
            jax.ShapeDtypeStruct((groups, pieces, capacity), jnp.bfloat16),
            jax.ShapeDtypeStruct(early.shape, jnp.bfloat16),
        ),
        in_specs=[pl.BlockSpec(memory_space=pl.ANY)] * 2,
        out_specs=(pl.BlockSpec(memory_space=pl.ANY),) * 2,
        scratch_shapes=[
            block, block, block, block,
            pltpu.VMEM((pieces, slots), jnp.bfloat16),
            pltpu.SemaphoreType.DMA((stack,)),
            pltpu.SemaphoreType.DMA((stack,)),
            pltpu.SemaphoreType.DMA((stack,)),
            pltpu.SemaphoreType.DMA((stack,)),
            pltpu.SemaphoreType.DMA((stack,)),
            pltpu.SemaphoreType.DMA((groups - 1,)),
            pltpu.SemaphoreType.DMA((groups - 1,)),
            pltpu.SemaphoreType.DMA((groups - 1,)),
            pltpu.SemaphoreType.DMA((groups - 1,)),
            pltpu.SemaphoreType.DMA,
        ],
        compiler_params=pltpu.CompilerParams(
            collective_id=collective, has_side_effects=True, vmem_limit_bytes=20 * 1024 * 1024
        ),
        cost_estimate=pl.CostEstimate(
            flops=sent, bytes_accessed=32 * sent, transcendentals=0
        ),
    )(partial, early)


def fused_device(
    hidden_states, norm_gain, gate_master, up_master, down_master, expert_ids, route_logits
):
    groups = lax.axis_size("tp")
    row_groups = lax.axis_size("fs")
    experts = gate_master.shape[0]
    local_count = experts // groups
    tokens, pieces = hidden_states.shape
    model_width = pieces * row_groups
    capacity = tokens // 2
    me = lax.axis_index("tp")
    gain = norm_gain[:, None]
    id_rows = expert_ids.size // pieces
    sheet = expert_ids.astype(jnp.bfloat16).reshape(id_rows, pieces)
    sheet = jnp.pad(sheet, ((0, -id_rows % 16), (0, 0)))
    everything = lax.all_gather(jnp.concatenate([hidden_states, sheet]), ("fs", "tp"), axis=0)
    everything = everything.reshape(row_groups, groups, -1, pieces)
    all_ids = everything[0, :, tokens : tokens + id_rows].astype(jnp.int32)
    all_ids = all_ids.reshape(groups, tokens, 2)
    raw = jnp.transpose(everything[:, :, :tokens], (1, 2, 0, 3)).reshape(groups, tokens, model_width)
    earlier = (jnp.arange(tokens)[:, None] > jnp.arange(tokens)[None, :]).astype(jnp.bfloat16)
    weights = jax.nn.softmax(route_logits, axis=1)
    named = expert_ids[:, :, None] == jnp.arange(experts, dtype=jnp.int32)[None, None, :]
    chosen = jnp.any(named, axis=1).astype(jnp.bfloat16)
    before = jnp.dot(earlier, chosen, preferred_element_type=jnp.float32)
    position = jnp.sum(jnp.where(named, before[:, None, :], 0.0), axis=2).astype(jnp.int32)
    slot_ids = (expert_ids * capacity + position).reshape(-1)

    dep = hidden_states
    served = []
    partials = []
    for j in range(local_count):
        gate, up, down = exchange(gain, gate_master, up_master, down_master, dep, j, 1 + j)
        served.append((gate, up, down))
        mine = jnp.any(all_ids == me * local_count + j, axis=2)
        spot = jnp.einsum(
            "ts,gs->gt", earlier, mine.astype(jnp.bfloat16), preferred_element_type=jnp.float32
        ).astype(jnp.int32)
        table = (
            mine[:, None, :]
            & (spot[:, None, :] == jnp.arange(capacity, dtype=jnp.int32)[None, :, None])
        ).astype(jnp.bfloat16)
        packed = jnp.einsum("gct,gtd->gcd", table, raw, preferred_element_type=jnp.float32)
        packed = packed.reshape(groups * capacity, model_width)
        mean = jnp.mean(packed * packed, axis=1, keepdims=True)
        normed = (packed * lax.rsqrt(mean + EPSILON)).astype(jnp.bfloat16)
        gate_pre = jnp.dot(normed, gate, preferred_element_type=jnp.float32)
        up_pre = jnp.dot(normed, up, preferred_element_type=jnp.float32)
        act = (jax.nn.silu(gate_pre) * up_pre).astype(jnp.bfloat16)
        partial = jnp.einsum(
            "dh,sh->ds", down, act, preferred_element_type=jnp.float32
        ).astype(jnp.bfloat16)
        partials.append(partial)
        dep = partial
    early = [
        lax.psum_scatter(partial, "fs", scatter_dimension=0, tiled=True)
        for partial in partials[:-1]
    ]
    early = jnp.stack([jnp.swapaxes(one.reshape(pieces, groups, capacity), 0, 1) for one in early], 1)
    last, early = gather_sum(partials[-1], early, 1 + local_count)
    ordered = jnp.concatenate([early, last[:, None]], axis=1)
    flat_out = jnp.moveaxis(ordered, 2, 0).reshape(pieces, experts * capacity)
    picked = flat_out.at[:, slot_ids].get(mode="promise_in_bounds")
    picked = picked.reshape(pieces, tokens, 2).astype(jnp.float32)
    combined = jnp.sum(picked * weights[None, :, :], axis=2)
    return tuple(jnp.stack([one[w] for one in served]) for w in range(3)) + (
        jnp.transpose(combined).astype(jnp.bfloat16),
    )


def arrange(weights, groups, row_groups):
    experts, rows, columns = weights.shape
    blocks = row_groups // groups
    split = weights.reshape(experts // groups, groups, rows, blocks, columns // blocks)
    split = split.reshape(groups, experts // groups, rows, blocks, columns // blocks)
    return jnp.transpose(split, (0, 3, 1, 2, 4))


def regroup(moved, row_groups):
    return moved.reshape((row_groups,) + moved.shape[2:])


def settle(arrived):
    return arrived.reshape(arrived.shape[1], arrived.shape[2], arrived.shape[3])


def per_device(
    hidden_states, norm_gain, gate_master, up_master, down_master, expert_ids, route_logits
):
    groups = lax.axis_size("tp")
    row_groups = lax.axis_size("fs")
    whole_tiles = gate_master.shape[2] // (row_groups // groups) % 128 == 0
    if whole_tiles and gate_master.shape[0] > groups and row_groups % 4 == 0 and expert_ids.size % hidden_states.shape[1] == 0:
        return fused_device(
            hidden_states, norm_gain, gate_master, up_master, down_master, expert_ids, route_logits
        )
    experts = gate_master.shape[0]
    local_count = experts // groups
    tokens = hidden_states.shape[0]
    pieces = hidden_states.shape[1]
    model_width = pieces * row_groups
    capacity = tokens // 2
    scaled = norm_gain[None, :, None]
    gate_cast = arrange((scaled * gate_master).astype(jnp.bfloat16), groups, row_groups)
    up_cast = arrange((scaled * up_master).astype(jnp.bfloat16), groups, row_groups)
    down_cast = arrange(down_master.astype(jnp.bfloat16), groups, row_groups)
    sectioned = (
        lax.all_to_all(gate_cast, "tp", split_axis=0, concat_axis=0, tiled=True),
        lax.all_to_all(up_cast, "tp", split_axis=0, concat_axis=0, tiled=True),
        lax.all_to_all(down_cast, "tp", split_axis=0, concat_axis=0, tiled=True),
    )
    landed = (
        lax.all_to_all(
            regroup(sectioned[0], row_groups), "fs", split_axis=0, concat_axis=2, tiled=True
        ),
        lax.all_to_all(
            regroup(sectioned[1], row_groups), "fs", split_axis=0, concat_axis=2, tiled=True
        ),
        lax.all_to_all(
            regroup(sectioned[2], row_groups), "fs", split_axis=0, concat_axis=2, tiled=True
        ),
    )
    gate_serve, up_serve, down_serve = (settle(landed[0]), settle(landed[1]), settle(landed[2]))
    values = hidden_states.astype(jnp.float32)
    squares = lax.psum(jnp.sum(values * values, axis=1), "fs")
    normed = (values * lax.rsqrt(squares / model_width + EPSILON)[:, None]).astype(jnp.bfloat16)
    weights = jax.nn.softmax(route_logits, axis=1)
    chosen = (expert_ids[:, :, None] == jnp.arange(experts, dtype=jnp.int32)[None, None, :]).astype(
        jnp.int32
    )
    chosen = chosen.reshape(tokens * 2, experts)
    before = jnp.cumsum(chosen, axis=0) - chosen
    position = jnp.sum(before * chosen, axis=1)
    slot_ids = expert_ids.reshape(-1) * capacity + position
    slot_table = (
        slot_ids[None, :] == jnp.arange(experts * capacity, dtype=jnp.int32)[:, None]
    ).astype(jnp.bfloat16)
    dispatch = jnp.sum(slot_table.reshape(experts * capacity, tokens, 2), axis=2)
    whole_rows = lax.all_gather(normed, "fs", axis=1, tiled=True)
    packed = jnp.dot(dispatch, whole_rows, preferred_element_type=jnp.float32).astype(jnp.bfloat16)
    arrived = lax.all_to_all(
        packed.reshape(groups, local_count * capacity, model_width),
        "tp",
        split_axis=0,
        concat_axis=0,
        tiled=True,
    )
    arranged = arrived.reshape(groups, local_count, capacity, model_width)
    activations = []
    for expert_index in range(local_count):
        expert_rows = arranged[:, expert_index].reshape(groups * capacity, model_width)
        gate_pre = jnp.dot(
            expert_rows, gate_serve[expert_index], preferred_element_type=jnp.float32
        )
        up_pre = jnp.dot(expert_rows, up_serve[expert_index], preferred_element_type=jnp.float32)
        activations.append((jax.nn.silu(gate_pre) * up_pre).astype(jnp.bfloat16))
    stacked = jnp.stack(activations)
    summed = lax.psum_scatter(
        jnp.einsum("jdh,jsh->djs", down_serve, stacked, preferred_element_type=jnp.float32).astype(
            jnp.bfloat16
        ),
        "fs",
        scatter_dimension=0,
        tiled=True,
    )
    results = summed.reshape(pieces, local_count, groups, capacity)
    returned = lax.all_to_all(results, "tp", split_axis=2, concat_axis=1, tiled=True)
    flat_out = returned.reshape(pieces, experts * capacity)
    picked = jnp.take(flat_out, slot_ids, axis=1).reshape(pieces, tokens, 2).astype(jnp.float32)
    combined = jnp.sum(picked * weights[None, :, :], axis=2)
    return (gate_serve, up_serve, down_serve, jnp.transpose(combined).astype(jnp.bfloat16))


def solution(mesh):
    in_specs = (
        P("tp", "fs"),
        P("fs"),
        P(None, "fs", "tp"),
        P(None, "fs", "tp"),
        P(None, "fs", "tp"),
        P("tp", None),
        P("tp", None),
    )
    out_specs = (P("tp", None, "fs"), P("tp", None, "fs"), P("tp", None, "fs"), P("tp", "fs"))
    return jax.shard_map(
        per_device, mesh=mesh, in_specs=in_specs, out_specs=out_specs, check_vma=False
    )
```
